32 devices in a mesh: sp: 8 (over z, x), tp: 4 (over y, core).
Axes of the slice: x: 2, y: 2, z: 4, core: 2. Of those that a mesh axis runs over, the one named last changes fastest.
Arguments:
- tokens: bfloat16 [2048, 2048], P(('sp', 'tp')), may hold values from -6 to 6
- query_weight: bfloat16 [2048, 2048], P('sp', 'tp'), may hold values from -0.125 to 0.125
- key_weight: bfloat16 [2048, 512], P('sp', 'tp'), may hold values from -0.125 to 0.125
- value_weight: bfloat16 [2048, 512], P('sp', 'tp'), may hold values from -0.125 to 0.125
- out_weight: bfloat16 [2048, 2048], P('tp', 'sp'), may hold values from -0.125 to 0.125
- query_gain: float32 [128], replicated, may hold values from 0.1 to 1.9
- key_gain: float32 [128], replicated, may hold values from 0.1 to 1.9
Outputs:
- mixed: bfloat16 [2048, 2048], P(('sp', 'tp'))
The draws below stay inside these ranges and needn't reach their ends.
All inputs are finite; a program needn't handle non-finite values.
Results may differ from the reference program's by a relative error of at most 0.02.
Values may be sent and summed in bfloat16 or wider, within the bound.
A program may use at most 64 MiB of HBM per device.

```python
import math
import jax
import jax.numpy as jnp
from jax import lax

D = 2048
HEAD_DIM = 128
Q_HEADS = 16
KV_HEADS = 4
GROUP = 4
GRID_W = 64
TOKENS = 2048


def block_scale(rng, shape, cuts, least, high):
    level, own = 1.0, jax.random.fold_in(rng, 6)
    for position, blocks in cuts:
        heights = jnp.exp(jax.random.uniform(jax.random.fold_in(own, position), (blocks,), jnp.float32, least / len(cuts), high / len(cuts)))
        level = level * jnp.repeat(heights, shape[position] // blocks).reshape([-1 if axis == position else 1 for axis in range(len(shape))])
    return level


def noise(rng, extent, width, bound, shards=(), held_as=jnp.bfloat16):
    result = jax.random.normal(rng, extent, jnp.float32) * width
    if len(shards) > 0:
        result = block_scale(rng, extent, shards, -0.22, 0.18) * result
    return jnp.clip(result, min=-bound, max=bound).astype(held_as)


def setup_inputs(seed: int = 0) -> dict:
    key_list = jax.random.split(jax.random.key(seed), 8)
    tokens = noise(key_list[0], (TOKENS, D), 1.0, 6.0, ((0, 32),))
    query_weight = noise(key_list[1], (D, Q_HEADS * HEAD_DIM), D ** -0.5, 0.125, ((0, 8), (1, 4)))
    key_weight = noise(key_list[2], (D, KV_HEADS * HEAD_DIM), D ** -0.5, 0.125, ((0, 8), (1, 4)))
    value_weight = noise(key_list[3], (D, KV_HEADS * HEAD_DIM), D ** -0.5, 0.125, ((0, 8), (1, 4)))
    out_weight = noise(key_list[4], (Q_HEADS * HEAD_DIM, D), (Q_HEADS * HEAD_DIM) ** -0.5, 0.125, ((0, 4), (1, 8)))
    query_gain = jnp.clip(1.0 + 0.18 * jax.random.normal(key_list[5], (HEAD_DIM,), jnp.float32), 0.1, 1.9)
    key_gain = jnp.clip(1.0 + 0.18 * jax.random.normal(key_list[6], (HEAD_DIM,), jnp.float32), 0.1, 1.9)
    return dict(tokens=tokens, query_weight=query_weight, key_weight=key_weight, value_weight=value_weight, out_weight=out_weight, query_gain=query_gain, key_gain=key_gain)


eps = 1e-06
rope_base = 10000.0

def normalize(raw, gain):
    wide = raw.astype(jnp.float32)
    return wide * lax.rsqrt(lax.optimization_barrier(jnp.mean(wide * wide, axis=-1, keepdims=True)) + eps) * gain

def rotate(values_in, positions):
    pair_count = values_in.shape[-1] // 4
    inverse_rate = rope_base ** (-jnp.arange(0, 2 * pair_count, 2, dtype=jnp.float32) / (2 * pair_count))
    grid_row = (positions // GRID_W).astype(jnp.float32)
    grid_column = (positions % GRID_W).astype(jnp.float32)
    angles = jnp.stack([grid_row[:, None] * inverse_rate, grid_column[:, None] * inverse_rate], axis=1)
    cosine = jnp.cos(angles)[:, None]
    sine = jnp.sin(angles)[:, None]
    shaped = values_in.reshape(values_in.shape[:-1] + (2, 2, pair_count))
    leading = shaped[..., 0, :]
    trailing = shaped[..., 1, :]
    turned = jnp.stack([leading * cosine - trailing * sine, trailing * cosine + leading * sine], axis=-2)
    return turned.reshape(values_in.shape)

def reference(tokens, query_weight, key_weight, value_weight, out_weight, query_gain, key_gain):
    rows = tokens.shape[0]

    def project(weight, heads):
        return jnp.dot(tokens, weight, preferred_element_type=jnp.float32).astype(jnp.bfloat16).reshape(rows, heads, HEAD_DIM)
    positions = jnp.arange(rows, dtype=jnp.int32)
    queries = rotate(normalize(project(query_weight, Q_HEADS), query_gain), positions).astype(jnp.bfloat16)
    keys = rotate(normalize(project(key_weight, KV_HEADS), key_gain), positions).astype(jnp.bfloat16)
    values = project(value_weight, KV_HEADS)
    block = math.gcd(rows, 128)
    grouped = queries.reshape(rows // block, block, KV_HEADS, GROUP, HEAD_DIM)
    scale = HEAD_DIM ** (-0.5)

    def one_block(query_block):
        scores = jnp.einsum('qkgd,skd->kgqs', query_block, keys, preferred_element_type=jnp.float32) * scale
        highest = lax.optimization_barrier(jnp.max(scores, axis=-1, keepdims=True))
        exponentials = jnp.exp(scores - highest)
        total = lax.optimization_barrier(jnp.sum(exponentials, axis=-1))
        weights = exponentials.astype(jnp.bfloat16)
        summed = jnp.einsum('kgqs,skd->kgqd', weights, values, preferred_element_type=jnp.float32)
        return jnp.transpose(summed / total[..., None], (2, 0, 1, 3))
    attended = lax.map(one_block, grouped).reshape(rows, Q_HEADS * HEAD_DIM).astype(jnp.bfloat16)
    projected = jnp.dot(attended, out_weight, preferred_element_type=jnp.float32)
    scaled = projected * lax.rsqrt(lax.optimization_barrier(jnp.mean(projected * projected, axis=-1, keepdims=True)) + eps)
    return scaled.astype(jnp.bfloat16)
```

```python
import functools
import math

import jax
import jax.numpy as jnp
from jax import lax
from jax.experimental import pallas as pl
from jax.experimental.pallas import tpu as pltpu
from jax.sharding import PartitionSpec as P

HEAD_DIM = 128
GRID_W = 64
MESH = pl.DeviceIdType.MESH

eps = 1e-06
rope_base = 10000.0
BLOCK = 256
NT = (((1,), (1,)), ((), ()))


def remote(src, dst, send_sem, recv_sem, device):
    return pltpu.make_async_remote_copy(
        src_ref=src,
        dst_ref=dst,
        send_sem=send_sem,
        recv_sem=recv_sem,
        device_id=device,
        device_id_type=MESH,
    )


class Line:
    def __init__(self, own, buffer, size, send, recv, s, t, lines):
        self.own, self.buffer, self.size = own, buffer, size
        self.send, self.recv, self.s, self.t, self.lines = send, recv, s, t, lines
        self.line, self.half = s // 2, lax.rem(s, 2)

    def place(self, source):
        return self.buffer.at[pl.ds(pl.multiple_of(source * self.size, self.size), self.size)]

    def along(self, source, way, src=None):
        where = self.place(source)
        return remote(
            where if src is None else src,
            where,
            self.send.at[way, source],
            self.recv.at[source],
            (self.s + (2 if way else -2), self.t),
        )

    def push(self, source, way, src=None):
        @pl.when(self.line < self.lines - 1 if way else self.line > 0)
        def _():
            self.along(source, way, src).start()

    def pair(self):
        return remote(
            self.own.at[1 - self.half],
            self.place(self.s),
            self.send.at[2, self.s],
            self.recv.at[self.s],
            (self.s + 1 - 2 * self.half, self.t),
        )

    def local(self):
        return pltpu.make_async_copy(
            self.own.at[self.half], self.place(self.s), self.send.at[2, self.s + 1 - 2 * self.half]
        )

    def push_own(self):
        self.push(self.s, 0, self.own.at[self.half])
        self.push(self.s, 1, self.own.at[self.half])

    def arrived(self, source):
        self.along(source, 0).wait_recv()

    def push_pair(self):
        other = self.s + 1 - 2 * self.half
        self.arrived(other)
        self.push(other, 0)
        self.push(other, 1)

    def step(self, distance):
        for j in range(2):
            @pl.when(self.line >= distance)
            def _():
                source = 2 * (self.line - distance) + j
                self.arrived(source)
                self.push(source, 1)

            @pl.when(self.line + distance < self.lines)
            def _():
                source = 2 * (self.line + distance) + j
                self.arrived(source)
                self.push(source, 0)

    def finish(self):
        self.pair().wait_send()

        def one(source, _):
            @pl.when((source // 2 <= self.line) & (self.line < self.lines - 1))
            def _():
                self.along(source, 1).wait_send()

            @pl.when((source // 2 >= self.line) & (self.line > 0))
            def _():
                self.along(source, 0).wait_send()

            return 0

        lax.fori_loop(0, 2 * self.lines, one, 0)


def kernel(
    S, T,
    x_ref, w_ref, o_ref, qg_ref, kg_ref, out_ref,
    X, W, OW, KV, Q, A, C, SN, best, total, summed, PS, SB, RC, SF, RF,
    xs_sem, xr_sem, ws_sem, wr_sem, os_sem, or_sem, ks_sem, kr_sem, kp_sem, kq_sem,
    cs_sem, fs_sem, fr_sem,
):
    L, N = S // 2, 2 * T
    R, D = x_ref.shape
    M = N * R
    wr, wc = w_ref.shape[1:]
    oc, hw = o_ref.shape[1:]
    heads = hw // HEAD_DIM
    s, t = lax.axis_index("sp"), lax.axis_index("tp")
    line, half = s // 2, lax.rem(s, 2)
    core, across = lax.rem(t, 2), t // 2
    mate = t + 1 - 2 * core
    other = s + 1 - 2 * half
    H = T // 2
    slot = half * T + t
    h = half * H + across

    def plane(b):
        return (2 * line + b // T, lax.rem(b, T))

    barrier = pltpu.get_barrier_semaphore()
    for i in range(1, N):
        pl.semaphore_signal(
            barrier, inc=1, device_id=plane(lax.rem(slot + i, N)), device_id_type=MESH
        )

    @pl.when(line > 0)
    def _():
        pl.semaphore_signal(barrier, inc=1, device_id=(s - 2, t), device_id_type=MESH)

    @pl.when(line < L - 1)
    def _():
        pl.semaphore_signal(barrier, inc=1, device_id=(s + 2, t), device_id_type=MESH)

    pl.semaphore_wait(
        barrier,
        N - 1 + jnp.where(line > 0, 1, 0) + jnp.where(line < L - 1, 1, 0),
    )

    weights = Line(w_ref, W, wr, ws_sem, wr_sem, s, t, L)
    outs = Line(o_ref, OW, oc, os_sem, or_sem, s, t, L)

    def rows(b):
        return X.at[pl.ds(pl.multiple_of(b * R, R), R)]

    def peer(hh):
        return hh // H, 2 * lax.rem(hh, H) + core

    def token_send(i):
        ph, pt = peer(lax.rem(h + i, T))
        return remote(x_ref, rows(slot), xs_sem.at[i], xr_sem.at[slot], (2 * line + ph, pt))

    def token_block(i):
        ph, pt = peer(lax.rem(h + T - i, T))
        return ph * T + pt

    def token_mate(i):
        b = token_block(i)
        return remote(
            x_ref if i == 0 else rows(b), rows(b), xs_sem.at[T + i], xr_sem.at[b], (s, mate)
        )

    weights.pair().start()
    weights.push_own()
    for i in range(1, T):
        token_send(i).start()
    token_mate(0).start()
    outs.pair().start()
    weights.local().start()
    outs.local().start()
    own_tokens = pltpu.make_async_copy(x_ref, rows(slot), xs_sem.at[0])
    own_tokens.start()

    lane = lax.broadcasted_iota(jnp.int32, (BLOCK, HEAD_DIM), 1)
    pairs = HEAD_DIM // 4
    rate = jnp.exp(
        lax.rem(lane, pairs).astype(jnp.float32) * (-math.log(rope_base) / pairs)
    )
    by_row = lane < 2 * pairs
    leading = lax.rem(lane, 2 * pairs) < pairs
    for rb in range(M // BLOCK):
        position = (
            line * M + rb * BLOCK + lax.broadcasted_iota(jnp.int32, (BLOCK, HEAD_DIM), 0)
        )
        grid = jnp.where(by_row, position // GRID_W, lax.rem(position, GRID_W))
        angle = grid.astype(jnp.float32) * rate
        C[pl.ds(rb * BLOCK, BLOCK), :] = jnp.cos(angle)
        sine = jnp.sin(angle)
        SN[pl.ds(rb * BLOCK, BLOCK), :] = jnp.where(leading, -sine, sine)
    best[...] = jnp.full_like(best, -jnp.inf)
    total[...] = jnp.zeros_like(total)
    summed[...] = jnp.zeros_like(summed)

    weights.push_pair()
    weights.step(1)
    for i in range(1, T):
        remote(x_ref, rows(token_block(i)), xs_sem.at[i], xr_sem.at[token_block(i)], (s, mate)).wait_recv()
        token_mate(i).start()

    def weight_step(d, _):
        weights.step(d)
        return 0

    lax.fori_loop(2, L, weight_step, 0)
    outs.push_own()
    outs.push_pair()
    own_tokens.wait()
    weights.local().wait()
    outs.local().wait()

    def mate_block(i):
        hh = lax.rem(h + T - i, T)
        return (hh // H) * T + 2 * lax.rem(hh, H) + 1 - core

    for i in range(T):
        b = mate_block(i)
        remote(x_ref, rows(b), xs_sem.at[i], xr_sem.at[b], (s, mate)).wait_recv()

    def turned(raw, gain, at):
        n = raw * lax.rsqrt(jnp.mean(raw * raw, axis=-1, keepdims=True) + eps) * gain
        partner = jnp.where(
            leading, pltpu.roll(n, HEAD_DIM - pairs, 1), pltpu.roll(n, pairs, 1)
        )
        return (n * C[at, :] + partner * SN[at, :]).astype(jnp.bfloat16)

    for rb in range(M // BLOCK):
        at = pl.ds(rb * BLOCK, BLOCK)
        raw = jnp.dot(X[at, :], W[...], preferred_element_type=jnp.float32).astype(jnp.bfloat16)
        mine = pl.ds(pl.multiple_of(line * M + rb * BLOCK, BLOCK), BLOCK)
        kv = raw[:, hw:]

        @pl.when(half == 0)
        def _():
            KV[0, mine, :] = turned(kv.astype(jnp.float32), kg_ref[...], at)

        @pl.when(half == 1)
        def _():
            KV[1, mine, :] = kv

        for j in range(heads):
            part = raw[:, j * HEAD_DIM : (j + 1) * HEAD_DIM].astype(jnp.float32)
            Q[pl.ds(j * M + rb * BLOCK, BLOCK), :] = turned(part, qg_ref[...], at)

    def chunk(which, source):
        return KV.at[which, pl.ds(pl.multiple_of(source * M, M), M)]

    def kv_along(source, way):
        return remote(
            chunk(half, source), chunk(half, source), ks_sem.at[way, source], kr_sem.at[source],
            (s + (2 if way else -2), t),
        )

    def kv_pair(source, which):
        return remote(
            chunk(which, source), chunk(which, source), kp_sem.at[source], kq_sem.at[source],
            (other, t),
        )

    def kv_push(source, way):
        @pl.when(line < L - 1 if way else line > 0)
        def _():
            kv_along(source, way).start()

    def kv_step(d):
        for way in (1, 0):
            source = line - d if way else line + d

            @pl.when(line >= d if way else line + d < L)
            def _():
                kv_along(source, way).wait_recv()
                kv_push(source, way)
                kv_pair(source, half).start()

    factor = HEAD_DIM ** (-0.5) * math.log2(math.e)

    def attend(source):
        kv_pair(source, 1 - half).wait_recv()
        at = pl.ds(pl.multiple_of(source * M, M), M)

        def one(r, _):
            q_at = pl.ds(pl.multiple_of(r * BLOCK, BLOCK), BLOCK)
            scores = (
                lax.dot_general(Q[q_at, :], KV[0, at, :], NT, preferred_element_type=jnp.float32)
                * factor
            )
            old = best[q_at, :]
            fresh = jnp.maximum(old, jnp.max(scores, axis=-1, keepdims=True))
            shrink = jnp.exp2(old - fresh)
            exponentials = jnp.exp2(scores - fresh)
            best[q_at, :] = fresh
            total[q_at, :] = total[q_at, :] * shrink + jnp.sum(exponentials, axis=-1, keepdims=True)
            summed[q_at, :] = summed[q_at, :] * shrink + jnp.dot(
                exponentials.astype(jnp.bfloat16), KV[1, at, :], preferred_element_type=jnp.float32
            )
            return 0

        lax.fori_loop(0, heads * M // BLOCK, one, 0)

    def attend_at(d):
        @pl.when(line >= d)
        def _():
            attend(line - d)

        @pl.when(line + d < L)
        def _():
            attend(line + d)

    kv_push(line, 0)
    kv_push(line, 1)
    kv_pair(line, half).start()
    kv_step(1)
    attend(line)

    def kv_round(d, _):
        kv_step(d)
        attend_at(d - 1)
        return 0

    lax.fori_loop(2, L, kv_round, 0)
    outs.step(1)
    attend_at(L - 1)

    def out_round(d, _):
        outs.step(d)
        return 0

    lax.fori_loop(2, L, out_round, 0)

    for ph in range(2):
        for pt in range(T):
            source = (ph * T + pt) * R
            target = (pt % 2) * T * R + (ph * H + pt // 2) * R
            for j in range(heads):
                at = pl.ds(j * M + source, R)
                A[pl.ds(target, R), j * HEAD_DIM : (j + 1) * HEAD_DIM] = (
                    summed[at, :] / total[at, :]
                ).astype(jnp.bfloat16)

    TR = T * R
    width = min(D, 512)

    def product(parity, cb):
        return lax.dot_general(
            A[pl.ds(pl.multiple_of(parity * TR, TR), TR), :],
            OW[pl.ds(cb * width, width), :],
            NT,
            preferred_element_type=jnp.float32,
        )

    to_mate = remote(SB, RC, cs_sem.at[0], cs_sem.at[1], (s, mate))
    for cb in range(D // width):
        SB[:, cb * width : (cb + 1) * width] = product(1 - core, cb).astype(jnp.bfloat16)
    to_mate.start()
    for cb in range(D // width):
        PS[:, cb * width : (cb + 1) * width] = product(core, cb)
    to_mate.wait_recv()

    def final_send(i):
        ph, pt = peer(lax.rem(h + i, T))
        return remote(
            SF.at[i - 1], RF.at[i - 1], fs_sem.at[i - 1], fr_sem.at[i - 1], (2 * line + ph, pt)
        )

    def reduced(hh):
        at = pl.ds(pl.multiple_of(hh * R, R), R)
        return PS[at, :] + RC[at, :].astype(jnp.float32)

    for i in range(1, T):
        SF[i - 1] = reduced(lax.rem(h + i, T)).astype(jnp.bfloat16)
        final_send(i).start()
    result = reduced(h)
    for i in range(1, T):
        final_send(i).wait_recv()
        result = result + RF[i - 1].astype(jnp.float32)
    out_ref[...] = (
        result * lax.rsqrt(jnp.mean(result * result, axis=-1, keepdims=True) + eps)
    ).astype(out_ref.dtype)

    weights.finish()
    outs.finish()
    for i in range(1, T):
        token_send(i).wait_send()
        final_send(i).wait_send()
    for i in range(T):
        token_mate(i).wait_send()
    to_mate.wait_send()

    def kv_done(source, _):
        kv_pair(source, half).wait_send()

        @pl.when((source <= line) & (line < L - 1))
        def _():
            kv_along(source, 1).wait_send()

        @pl.when((source >= line) & (line > 0))
        def _():
            kv_along(source, 0).wait_send()

        return 0

    lax.fori_loop(0, L, kv_done, 0)


def per_device(tokens, query_weight, key_weight, value_weight, out_weight, query_gain, key_gain):
    S, T = lax.axis_size("sp"), lax.axis_size("tp")
    L = S // 2
    R, D = tokens.shape
    M = 2 * T * R
    hw = query_weight.shape[1] // 2
    heads = hw // HEAD_DIM
    wr, oc = query_weight.shape[0], out_weight.shape[1]
    wc = hw + HEAD_DIM
    w = jnp.stack(
        [
            jnp.concatenate([query_weight[:, :hw], key_weight], axis=1),
            jnp.concatenate([query_weight[:, hw:], value_weight], axis=1),
        ]
    )
    o = jnp.swapaxes(out_weight.reshape(2, hw, oc), 1, 2)
    vmem = pl.BlockSpec(memory_space=pltpu.VMEM)
    bf, f32 = jnp.bfloat16, jnp.float32
    dma = pltpu.SemaphoreType.DMA
    return pl.pallas_call(
        functools.partial(kernel, S, T),
        out_shape=jax.ShapeDtypeStruct((R, D), bf),
        in_specs=[vmem] * 5,
        out_specs=vmem,
        scratch_shapes=[
            pltpu.VMEM((M, D), bf),
            pltpu.VMEM((S * wr, wc), bf),
            pltpu.VMEM((S * oc, hw), bf),
            pltpu.VMEM((2, L * M, HEAD_DIM), bf),
            pltpu.VMEM((heads * M, HEAD_DIM), bf),
            pltpu.VMEM((M, hw), bf),
            pltpu.VMEM((M, HEAD_DIM), f32),
            pltpu.VMEM((M, HEAD_DIM), f32),
            pltpu.VMEM((heads * M, 1), f32),
            pltpu.VMEM((heads * M, 1), f32),
            pltpu.VMEM((heads * M, HEAD_DIM), f32),
            pltpu.VMEM((T * R, D), f32),
            pltpu.VMEM((T * R, D), bf),
            pltpu.VMEM((T * R, D), bf),
            pltpu.VMEM((T - 1, R, D), bf),
            pltpu.VMEM((T - 1, R, D), bf),
            dma((2 * T,)),
            dma((2 * T,)),
            dma((3, S)),
            dma((S,)),
            dma((3, S)),
            dma((S,)),
            dma((2, L)),
            dma((L,)),
            dma((L,)),
            dma((L,)),
            dma((2,)),
            dma((T - 1,)),
            dma((T - 1,)),
        ],
        compiler_params=pltpu.CompilerParams(collective_id=0, has_side_effects=True),
    )(tokens, w, o, query_gain.reshape(1, HEAD_DIM), key_gain.reshape(1, HEAD_DIM))


def solution(mesh):
    placed = (
        P(("sp", "tp"), None),
        P("sp", "tp"),
        P("sp", "tp"),
        P("sp", "tp"),
        P("tp", "sp"),
        P(),
        P(),
    )
    return jax.shard_map(
        per_device, mesh=mesh, in_specs=placed, out_specs=P(("sp", "tp"), None), check_vma=False
    )
```

```python
import functools
import math

import jax
import jax.numpy as jnp
from jax import lax
from jax.experimental import pallas as pl
from jax.experimental.pallas import tpu as pltpu
from jax.sharding import PartitionSpec as P

HEAD_DIM = 128
GRID_W = 64
MESH = pl.DeviceIdType.MESH

eps = 1e-06
rope_base = 10000.0
BLOCK = 256
NT = (((1,), (1,)), ((), ()))


def remote(src, dst, send_sem, recv_sem, device):
    return pltpu.make_async_remote_copy(
        src_ref=src,
        dst_ref=dst,
        send_sem=send_sem,
        recv_sem=recv_sem,
        device_id=device,
        device_id_type=MESH,
    )


class Line:
    def __init__(self, own, buffer, size, send, recv, s, t, lines):
        self.own, self.buffer, self.size = own, buffer, size
        self.send, self.recv, self.s, self.t, self.lines = send, recv, s, t, lines
        self.line, self.half = s // 2, lax.rem(s, 2)

    def place(self, source):
        return self.buffer.at[pl.ds(pl.multiple_of(source * self.size, self.size), self.size)]

    def along(self, source, way, src=None):
        where = self.place(source)
        return remote(
            where if src is None else src,
            where,
            self.send.at[way, source],
            self.recv.at[source],
            (self.s + (2 if way else -2), self.t),
        )

    def push(self, source, way, src=None):
        @pl.when(self.line < self.lines - 1 if way else self.line > 0)
        def _():
            self.along(source, way, src).start()

    def pair(self):
        return remote(
            self.own.at[1 - self.half],
            self.place(self.s),
            self.send.at[2, self.s],
            self.recv.at[self.s],
            (self.s + 1 - 2 * self.half, self.t),
        )

    def local(self):
        return pltpu.make_async_copy(
            self.own.at[self.half], self.place(self.s), self.send.at[2, self.s + 1 - 2 * self.half]
        )

    def push_own(self):
        self.push(self.s, 0, self.own.at[self.half])
        self.push(self.s, 1, self.own.at[self.half])

    def arrived(self, source):
        self.along(source, 0).wait_recv()

    def push_pair(self):
        other = self.s + 1 - 2 * self.half
        self.arrived(other)
        self.push(other, 0)
        self.push(other, 1)

    def step(self, distance):
        for j in range(2):
            @pl.when(self.line >= distance)
            def _():
                source = 2 * (self.line - distance) + j
                self.arrived(source)
                self.push(source, 1)

            @pl.when(self.line + distance < self.lines)
            def _():
                source = 2 * (self.line + distance) + j
                self.arrived(source)
                self.push(source, 0)

    def finish(self):
        self.pair().wait_send()

        def one(source, _):
            @pl.when((source // 2 <= self.line) & (self.line < self.lines - 1))
            def _():
                self.along(source, 1).wait_send()

            @pl.when((source // 2 >= self.line) & (self.line > 0))
            def _():
                self.along(source, 0).wait_send()

            return 0

        lax.fori_loop(0, 2 * self.lines, one, 0)


def kernel(
    S, T,
    x_ref, w_ref, v_ref, o_ref, qg_ref, kg_ref, out_ref,
    X, W, WV, OW, KV, Q, A, C, SN, best, total, summed, PS, SB, RC, SF, RF,
    xs_sem, xr_sem, ws_sem, wr_sem, vs_sem, vr_sem, os_sem, or_sem, ks_sem, kr_sem, kp_sem, kq_sem,
    cs_sem, cr_sem, fs_sem, fr_sem,
):
    L, N = S // 2, 2 * T
    R, D = x_ref.shape
    M = N * R
    wr = w_ref.shape[1]
    oc, hw = o_ref.shape[1:]
    heads = hw // HEAD_DIM
    s, t = lax.axis_index("sp"), lax.axis_index("tp")
    line, half = s // 2, lax.rem(s, 2)
    core, across = lax.rem(t, 2), t // 2
    mate = t + 1 - 2 * core
    other = s + 1 - 2 * half
    H = T // 2
    slot = half * T + t
    h = half * H + across

    def plane(b):
        return (2 * line + b // T, lax.rem(b, T))

    barrier = pltpu.get_barrier_semaphore()
    for i in range(1, N):
        pl.semaphore_signal(
            barrier, inc=1, device_id=plane(lax.rem(slot + i, N)), device_id_type=MESH
        )

    @pl.when(line > 0)
    def _():
        pl.semaphore_signal(barrier, inc=1, device_id=(s - 2, t), device_id_type=MESH)

    @pl.when(line < L - 1)
    def _():
        pl.semaphore_signal(barrier, inc=1, device_id=(s + 2, t), device_id_type=MESH)

    pl.semaphore_wait(
        barrier,
        N - 1 + jnp.where(line > 0, 1, 0) + jnp.where(line < L - 1, 1, 0),
    )

    weights = Line(w_ref, W, wr, ws_sem, wr_sem, s, t, L)
    kv_weights = Line(v_ref, WV, wr, vs_sem, vr_sem, s, t, L)
    outs = Line(o_ref, OW, oc, os_sem, or_sem, s, t, L)

    def rows(b):
        return X.at[pl.ds(pl.multiple_of(b * R, R), R)]

    def peer(hh):
        return hh // H, 2 * lax.rem(hh, H) + core

    def token_send(i):
        ph, pt = peer(lax.rem(h + i, T))
        return remote(x_ref, rows(slot), xs_sem.at[i], xr_sem.at[slot], (2 * line + ph, pt))

    def token_block(i):
        ph, pt = peer(lax.rem(h + T - i, T))
        return ph * T + pt

    def token_mate(i):
        b = token_block(i)
        return remote(
            x_ref if i == 0 else rows(b), rows(b), xs_sem.at[T + i], xr_sem.at[b], (s, mate)
        )

    kv_weights.pair().start()
    kv_weights.push_own()
    weights.pair().start()
    for i in range(1, T):
        token_send(i).start()
    token_mate(0).start()
    outs.pair().start()
    kv_weights.local().start()
    weights.local().start()
    outs.local().start()
    own_tokens = pltpu.make_async_copy(x_ref, rows(slot), xs_sem.at[0])
    own_tokens.start()

    lane = lax.broadcasted_iota(jnp.int32, (BLOCK, HEAD_DIM), 1)
    pairs = HEAD_DIM // 4
    rate = jnp.exp(
        lax.rem(lane, pairs).astype(jnp.float32) * (-math.log(rope_base) / pairs)
    )
    by_row = lane < 2 * pairs
    leading = lax.rem(lane, 2 * pairs) < pairs
    for rb in range(M // BLOCK):
        position = (
            line * M + rb * BLOCK + lax.broadcasted_iota(jnp.int32, (BLOCK, HEAD_DIM), 0)
        )
        grid = jnp.where(by_row, position // GRID_W, lax.rem(position, GRID_W))
        angle = grid.astype(jnp.float32) * rate
        C[pl.ds(rb * BLOCK, BLOCK), :] = jnp.cos(angle)
        sine = jnp.sin(angle)
        SN[pl.ds(rb * BLOCK, BLOCK), :] = jnp.where(leading, -sine, sine)
    best[...] = jnp.full_like(best, -jnp.inf)
    total[...] = jnp.zeros_like(total)
    summed[...] = jnp.zeros_like(summed)

    kv_weights.push_pair()

    def kv_weight_step(d, _):
        kv_weights.step(d)
        return 0

    lax.fori_loop(1, L - 1, kv_weight_step, 0)
    weights.push_own()
    weights.push_pair()
    kv_weights.step(L - 1)
    for i in range(1, T):
        remote(x_ref, rows(token_block(i)), xs_sem.at[i], xr_sem.at[token_block(i)], (s, mate)).wait_recv()
        token_mate(i).start()

    weights.step(1)
    own_tokens.wait()
    kv_weights.local().wait()

    def mate_block(i):
        hh = lax.rem(h + T - i, T)
        return (hh // H) * T + 2 * lax.rem(hh, H) + 1 - core

    for i in range(T):
        b = mate_block(i)
        remote(x_ref, rows(b), xs_sem.at[i], xr_sem.at[b], (s, mate)).wait_recv()

    def turned(raw, gain, at):
        n = raw * lax.rsqrt(jnp.mean(raw * raw, axis=-1, keepdims=True) + eps) * gain
        partner = jnp.where(
            leading, pltpu.roll(n, HEAD_DIM - pairs, 1), pltpu.roll(n, pairs, 1)
        )
        return (n * C[at, :] + partner * SN[at, :]).astype(jnp.bfloat16)

    for rb in range(M // BLOCK):
        at = pl.ds(rb * BLOCK, BLOCK)
        kv = jnp.dot(X[at, :], WV[...], preferred_element_type=jnp.float32).astype(jnp.bfloat16)
        mine = pl.ds(pl.multiple_of(line * M + rb * BLOCK, BLOCK), BLOCK)

        @pl.when(half == 0)
        def _():
            KV[0, mine, :] = turned(kv.astype(jnp.float32), kg_ref[...], at)

        @pl.when(half == 1)
        def _():
            KV[1, mine, :] = kv

    def chunk(which, source):
        return KV.at[which, pl.ds(pl.multiple_of(source * M, M), M)]

    def kv_along(source, way):
        return remote(
            chunk(half, source), chunk(half, source), ks_sem.at[way, source], kr_sem.at[source],
            (s + (2 if way else -2), t),
        )

    def kv_pair(source, which):
        return remote(
            chunk(which, source), chunk(which, source), kp_sem.at[source], kq_sem.at[source],
            (other, t),
        )

    def kv_push(source, way):
        @pl.when(line < L - 1 if way else line > 0)
        def _():
            kv_along(source, way).start()

    def kv_step(d):
        for way in (1, 0):
            source = line - d if way else line + d

            @pl.when(line >= d if way else line + d < L)
            def _():
                kv_along(source, way).wait_recv()
                kv_push(source, way)
                kv_pair(source, half).start()

    factor = HEAD_DIM ** (-0.5) * math.log2(math.e)

    def attend(source):
        kv_pair(source, 1 - half).wait_recv()
        at = pl.ds(pl.multiple_of(source * M, M), M)

        def one(r, _):
            q_at = pl.ds(pl.multiple_of(r * BLOCK, BLOCK), BLOCK)
            scores = (
                lax.dot_general(Q[q_at, :], KV[0, at, :], NT, preferred_element_type=jnp.float32)
                * factor
            )
            old = best[q_at, :]
            fresh = jnp.maximum(old, jnp.max(scores, axis=-1, keepdims=True))
            shrink = jnp.exp2(old - fresh)
            exponentials = jnp.exp2(scores - fresh)
            best[q_at, :] = fresh
            total[q_at, :] = total[q_at, :] * shrink + jnp.sum(exponentials, axis=-1, keepdims=True)
            summed[q_at, :] = summed[q_at, :] * shrink + jnp.dot(
                exponentials.astype(jnp.bfloat16), KV[1, at, :], preferred_element_type=jnp.float32
            )
            return 0

        lax.fori_loop(0, heads * M // BLOCK, one, 0)

    def attend_at(d):
        @pl.when(line >= d)
        def _():
            attend(line - d)

        @pl.when(line + d < L)
        def _():
            attend(line + d)

    kv_push(line, 0)
    kv_push(line, 1)
    kv_pair(line, half).start()

    def weight_step(d, _):
        kv_step(d - 1)
        weights.step(d)
        return 0

    lax.fori_loop(2, L, weight_step, 0)
    kv_step(L - 1)
    outs.push_own()
    outs.push_pair()
    weights.local().wait()
    outs.local().wait()
    for rb in range(M // BLOCK):
        at = pl.ds(rb * BLOCK, BLOCK)
        raw = jnp.dot(X[at, :], W[...], preferred_element_type=jnp.float32).astype(jnp.bfloat16)
        for j in range(heads):
            part = raw[:, j * HEAD_DIM : (j + 1) * HEAD_DIM].astype(jnp.float32)
            Q[pl.ds(j * M + rb * BLOCK, BLOCK), :] = turned(part, qg_ref[...], at)

    attend(line)
    outs.step(1)

    def attend_round(d, _):
        attend_at(d)
        return 0

    lax.fori_loop(1, L, attend_round, 0)

    for ph in range(2):
        for pt in range(T):
            source = (ph * T + pt) * R
            target = (pt % 2) * T * R + (ph * H + pt // 2) * R
            for j in range(heads):
                at = pl.ds(j * M + source, R)
                A[pl.ds(target, R), j * HEAD_DIM : (j + 1) * HEAD_DIM] = (
                    summed[at, :] / total[at, :]
                ).astype(jnp.bfloat16)

    TR = T * R
    width = 2 * oc

    def product(parity, g):
        return lax.dot_general(
            A[pl.ds(pl.multiple_of(parity * TR, TR), TR), :],
            OW[pl.ds(pl.multiple_of(g * width, width), width), :],
            NT,
            preferred_element_type=jnp.float32,
        )

    def to_mate(g):
        return remote(SB.at[g], RC.at[g], cs_sem.at[g], cr_sem.at[g], (s, mate))

    def final_send(g, i):
        ph, pt = peer(lax.rem(h + i, T))
        return remote(
            SF.at[g, i - 1], RF.at[g, i - 1], fs_sem.at[g, i - 1], fr_sem.at[g, i - 1],
            (2 * line + ph, pt),
        )

    def reduced(g, hh):
        at = pl.ds(pl.multiple_of(hh * R, R), R)
        return PS[g, at, :] + RC[g, at, :].astype(jnp.float32)

    def multiply(g):
        SB[g] = product(1 - core, g).astype(jnp.bfloat16)
        to_mate(g).start()
        PS[g] = product(core, g)

    def spread(g):
        to_mate(g).wait_recv()
        for i in range(1, T):
            SF[g, i - 1] = reduced(g, lax.rem(h + i, T)).astype(jnp.bfloat16)
            final_send(g, i).start()

    def both_ways(act, d):
        @pl.when(line >= d)
        def _():
            act(line - d)

        @pl.when(line + d < L)
        def _():
            act(line + d)

    multiply(line)
    both_ways(multiply, 1)
    spread(line)

    def out_round(d, _):
        both_ways(spread, d - 1)
        outs.step(d)
        both_ways(multiply, d)
        return 0

    lax.fori_loop(2, L, out_round, 0)
    both_ways(spread, L - 1)

    def gather_group(g, squares):
        result = reduced(g, h)
        for i in range(1, T):
            final_send(g, i).wait_recv()
            result = result + RF[g, i - 1].astype(jnp.float32)
        PS[g, pl.ds(pl.multiple_of(h * R, R), R), :] = result
        return squares + jnp.sum(result * result, axis=-1, keepdims=True)

    squares = lax.fori_loop(0, L, gather_group, jnp.zeros((R, 1), jnp.float32))
    norm = lax.rsqrt(squares / D + eps)
    for g in range(L):
        out_ref[:, g * width : (g + 1) * width] = (
            PS[g, pl.ds(pl.multiple_of(h * R, R), R), :] * norm
        ).astype(out_ref.dtype)

    kv_weights.finish()
    weights.finish()
    outs.finish()
    for i in range(1, T):
        token_send(i).wait_send()
    for i in range(T):
        token_mate(i).wait_send()

    def group_done(g, _):
        to_mate(g).wait_send()
        for i in range(1, T):
            final_send(g, i).wait_send()
        return 0

    lax.fori_loop(0, L, group_done, 0)

    def kv_done(source, _):
        kv_pair(source, half).wait_send()

        @pl.when((source <= line) & (line < L - 1))
        def _():
            kv_along(source, 1).wait_send()

        @pl.when((source >= line) & (line > 0))
        def _():
            kv_along(source, 0).wait_send()

        return 0

    lax.fori_loop(0, L, kv_done, 0)


def per_device(tokens, query_weight, key_weight, value_weight, out_weight, query_gain, key_gain):
    S, T = lax.axis_size("sp"), lax.axis_size("tp")
    L = S // 2
    R, D = tokens.shape
    M = 2 * T * R
    hw = query_weight.shape[1] // 2
    heads = hw // HEAD_DIM
    wr, oc = query_weight.shape[0], out_weight.shape[1]
    w = jnp.stack([query_weight[:, :hw], query_weight[:, hw:]])
    v = jnp.stack([key_weight, value_weight])
    o = jnp.swapaxes(out_weight.reshape(2, hw, oc), 1, 2)
    vmem = pl.BlockSpec(memory_space=pltpu.VMEM)
    bf, f32 = jnp.bfloat16, jnp.float32
    dma = pltpu.SemaphoreType.DMA
    return pl.pallas_call(
        functools.partial(kernel, S, T),
        out_shape=jax.ShapeDtypeStruct((R, D), bf),
        in_specs=[vmem] * 6,
        out_specs=vmem,
        scratch_shapes=[
            pltpu.VMEM((M, D), bf),
            pltpu.VMEM((S * wr, hw), bf),
            pltpu.VMEM((S * wr, HEAD_DIM), bf),
            pltpu.VMEM((S * oc, hw), bf),
            pltpu.VMEM((2, L * M, HEAD_DIM), bf),
            pltpu.VMEM((heads * M, HEAD_DIM), bf),
            pltpu.VMEM((M, hw), bf),
            pltpu.VMEM((M, HEAD_DIM), f32),
            pltpu.VMEM((M, HEAD_DIM), f32),
            pltpu.VMEM((heads * M, 1), f32),
            pltpu.VMEM((heads * M, 1), f32),
            pltpu.VMEM((heads * M, HEAD_DIM), f32),
            pltpu.VMEM((L, T * R, 2 * oc), f32),
            pltpu.VMEM((L, T * R, 2 * oc), bf),
            pltpu.VMEM((L, T * R, 2 * oc), bf),
            pltpu.VMEM((L, T - 1, R, 2 * oc), bf),
            pltpu.VMEM((L, T - 1, R, 2 * oc), bf),
            dma((2 * T,)),
            dma((2 * T,)),
            dma((3, S)),
            dma((S,)),
            dma((3, S)),
            dma((S,)),
            dma((3, S)),
            dma((S,)),
            dma((2, L)),
            dma((L,)),
            dma((L,)),
            dma((L,)),
            dma((L,)),
            dma((L,)),
            dma((L, T - 1)),
            dma((L, T - 1)),
        ],
        compiler_params=pltpu.CompilerParams(collective_id=0, has_side_effects=True),
    )(tokens, w, v, o, query_gain.reshape(1, HEAD_DIM), key_gain.reshape(1, HEAD_DIM))


def solution(mesh):
    placed = (
        P(("sp", "tp"), None),
        P("sp", "tp"),
        P("sp", "tp"),
        P("sp", "tp"),
        P("tp", "sp"),
        P(),
        P(),
    )
    return jax.shard_map(
        per_device, mesh=mesh, in_specs=placed, out_specs=P(("sp", "tp"), None), check_vma=False
    )
```

```python
import functools
import math

import jax
import jax.numpy as jnp
from jax import lax
from jax.experimental import pallas as pl
from jax.experimental.pallas import tpu as pltpu
from jax.sharding import PartitionSpec as P

HEAD_DIM = 128
GRID_W = 64
MESH = pl.DeviceIdType.MESH

eps = 1e-06
rope_base = 10000.0
BLOCK = 256
NT = (((1,), (1,)), ((), ()))


def remote(src, dst, send_sem, recv_sem, device):
    return pltpu.make_async_remote_copy(
        src_ref=src,
        dst_ref=dst,
        send_sem=send_sem,
        recv_sem=recv_sem,
        device_id=device,
        device_id_type=MESH,
    )


class Line:
    def __init__(self, own, buffer, size, send, recv, s, t, lines):
        self.own, self.buffer, self.size = own, buffer, size
        self.send, self.recv, self.s, self.t, self.lines = send, recv, s, t, lines
        self.line, self.half = s // 2, lax.rem(s, 2)

    def place(self, source):
        return self.buffer.at[pl.ds(pl.multiple_of(source * self.size, self.size), self.size)]

    def along(self, source, way, src=None):
        where = self.place(source)
        return remote(
            where if src is None else src,
            where,
            self.send.at[way, source],
            self.recv.at[source],
            (self.s + (2 if way else -2), self.t),
        )

    def push(self, source, way, src=None):
        @pl.when(self.line < self.lines - 1 if way else self.line > 0)
        def _():
            self.along(source, way, src).start()

    def pair(self):
        return remote(
            self.own.at[1 - self.half],
            self.place(self.s),
            self.send.at[2, self.s],
            self.recv.at[self.s],
            (self.s + 1 - 2 * self.half, self.t),
        )

    def local(self):
        return pltpu.make_async_copy(
            self.own.at[self.half], self.place(self.s), self.send.at[2, self.s + 1 - 2 * self.half]
        )

    def push_own(self):
        self.push(self.s, 0, self.own.at[self.half])
        self.push(self.s, 1, self.own.at[self.half])

    def arrived(self, source):
        self.along(source, 0).wait_recv()

    def push_pair(self):
        other = self.s + 1 - 2 * self.half
        self.arrived(other)
        self.push(other, 0)
        self.push(other, 1)

    def step(self, distance):
        for j in range(2):
            @pl.when(self.line >= distance)
            def _():
                source = 2 * (self.line - distance) + j
                self.arrived(source)
                self.push(source, 1)

            @pl.when(self.line + distance < self.lines)
            def _():
                source = 2 * (self.line + distance) + j
                self.arrived(source)
                self.push(source, 0)

    def finish(self):
        self.pair().wait_send()

        def one(source, _):
            @pl.when((source // 2 <= self.line) & (self.line < self.lines - 1))
            def _():
                self.along(source, 1).wait_send()

            @pl.when((source // 2 >= self.line) & (self.line > 0))
            def _():
                self.along(source, 0).wait_send()

            return 0

        lax.fori_loop(0, 2 * self.lines, one, 0)


def kernel(
    S, T,
    x_ref, w_ref, v_ref, o_ref, qg_ref, kg_ref, out_ref,
    X, W, WV, OW, KV, Q, A, C, SN, best, total, summed, PS, SB, RC, SF, RF,
    xs_sem, xr_sem, ws_sem, wr_sem, vs_sem, vr_sem, os_sem, or_sem, ks_sem, kr_sem, kp_sem, kq_sem,
    cs_sem, cr_sem, fs_sem, fr_sem,
):
    L, N = S // 2, 2 * T
    R, D = x_ref.shape
    M = N * R
    wr = w_ref.shape[1]
    oc, hw = o_ref.shape[1:]
    heads = hw // HEAD_DIM
    s, t = lax.axis_index("sp"), lax.axis_index("tp")
    line, half = s // 2, lax.rem(s, 2)
    core, across = lax.rem(t, 2), t // 2
    mate = t + 1 - 2 * core
    other = s + 1 - 2 * half
    H = T // 2
    slot = half * T + t
    h = half * H + across

    def plane(b):
        return (2 * line + b // T, lax.rem(b, T))

    barrier = pltpu.get_barrier_semaphore()
    for i in range(1, N):
        pl.semaphore_signal(
            barrier, inc=1, device_id=plane(lax.rem(slot + i, N)), device_id_type=MESH
        )

    @pl.when(line > 0)
    def _():
        pl.semaphore_signal(barrier, inc=1, device_id=(s - 2, t), device_id_type=MESH)

    @pl.when(line < L - 1)
    def _():
        pl.semaphore_signal(barrier, inc=1, device_id=(s + 2, t), device_id_type=MESH)

    pl.semaphore_wait(
        barrier,
        N - 1 + jnp.where(line > 0, 1, 0) + jnp.where(line < L - 1, 1, 0),
    )

    weights = Line(w_ref, W, wr, ws_sem, wr_sem, s, t, L)
    kv_weights = Line(v_ref, WV, wr, vs_sem, vr_sem, s, t, L)
    outs = Line(o_ref, OW, oc, os_sem, or_sem, s, t, L)

    def rows(b):
        return X.at[pl.ds(pl.multiple_of(b * R, R), R)]

    def peer(hh):
        return hh // H, 2 * lax.rem(hh, H) + core

    def token_send(i):
        ph, pt = peer(lax.rem(h + i, T))
        return remote(x_ref, rows(slot), xs_sem.at[i], xr_sem.at[slot], (2 * line + ph, pt))

    def token_block(i):
        ph, pt = peer(lax.rem(h + T - i, T))
        return ph * T + pt

    def token_mate(i):
        b = token_block(i)
        return remote(
            x_ref if i == 0 else rows(b), rows(b), xs_sem.at[T + i], xr_sem.at[b], (s, mate)
        )

    kv_weights.pair().start()
    kv_weights.push_own()
    weights.pair().start()
    for i in range(1, T):
        token_send(i).start()
    token_mate(0).start()
    outs.pair().start()
    kv_weights.local().start()
    weights.local().start()
    outs.local().start()
    own_tokens = pltpu.make_async_copy(x_ref, rows(slot), xs_sem.at[0])
    own_tokens.start()

    lane = lax.broadcasted_iota(jnp.int32, (BLOCK, HEAD_DIM), 1)
    pairs = HEAD_DIM // 4
    rate = jnp.exp(
        lax.rem(lane, pairs).astype(jnp.float32) * (-math.log(rope_base) / pairs)
    )
    by_row = lane < 2 * pairs
    leading = lax.rem(lane, 2 * pairs) < pairs
    for rb in range(M // BLOCK):
        position = (
            line * M + rb * BLOCK + lax.broadcasted_iota(jnp.int32, (BLOCK, HEAD_DIM), 0)
        )
        grid = jnp.where(by_row, position // GRID_W, lax.rem(position, GRID_W))
        angle = grid.astype(jnp.float32) * rate
        C[pl.ds(rb * BLOCK, BLOCK), :] = jnp.cos(angle)
        sine = jnp.sin(angle)
        SN[pl.ds(rb * BLOCK, BLOCK), :] = jnp.where(leading, -sine, sine)
    best[...] = jnp.full_like(best, -jnp.inf)
    total[...] = jnp.zeros_like(total)
    summed[...] = jnp.zeros_like(summed)

    kv_weights.push_pair()

    def kv_weight_step(d, _):
        kv_weights.step(d)
        return 0

    lax.fori_loop(1, L - 1, kv_weight_step, 0)
    weights.push_own()
    weights.push_pair()
    kv_weights.step(L - 1)
    for i in range(1, T):
        remote(x_ref, rows(token_block(i)), xs_sem.at[i], xr_sem.at[token_block(i)], (s, mate)).wait_recv()
        token_mate(i).start()

    weights.step(1)
    own_tokens.wait()
    kv_weights.local().wait()

    def mate_block(i):
        hh = lax.rem(h + T - i, T)
        return (hh // H) * T + 2 * lax.rem(hh, H) + 1 - core

    for i in range(T):
        b = mate_block(i)
        remote(x_ref, rows(b), xs_sem.at[i], xr_sem.at[b], (s, mate)).wait_recv()

    def turned(raw, gain, at):
        n = raw * lax.rsqrt(jnp.mean(raw * raw, axis=-1, keepdims=True) + eps) * gain
        partner = jnp.where(
            leading, pltpu.roll(n, HEAD_DIM - pairs, 1), pltpu.roll(n, pairs, 1)
        )
        return (n * C[at, :] + partner * SN[at, :]).astype(jnp.bfloat16)

    for rb in range(M // BLOCK):
        at = pl.ds(rb * BLOCK, BLOCK)
        kv = jnp.dot(X[at, :], WV[...], preferred_element_type=jnp.float32).astype(jnp.bfloat16)
        mine = pl.ds(pl.multiple_of(line * M + rb * BLOCK, BLOCK), BLOCK)

        @pl.when(half == 0)
        def _():
            KV[0, mine, :] = turned(kv.astype(jnp.float32), kg_ref[...], at)

        @pl.when(half == 1)
        def _():
            KV[1, mine, :] = kv

    def chunk(which, source):
        return KV.at[which, pl.ds(pl.multiple_of(source * M, M), M)]

    def kv_along(source, way):
        return remote(
            chunk(half, source), chunk(half, source), ks_sem.at[way, source], kr_sem.at[source],
            (s + (2 if way else -2), t),
        )

    def kv_pair(source, which):
        return remote(
            chunk(which, source), chunk(which, source), kp_sem.at[source], kq_sem.at[source],
            (other, t),
        )

    def kv_push(source, way):
        @pl.when(line < L - 1 if way else line > 0)
        def _():
            kv_along(source, way).start()

    def kv_step(d):
        for way in (1, 0):
            source = line - d if way else line + d

            @pl.when(line >= d if way else line + d < L)
            def _():
                kv_along(source, way).wait_recv()
                kv_push(source, way)
                kv_pair(source, half).start()

    factor = HEAD_DIM ** (-0.5) * math.log2(math.e)

    def attend(source):
        kv_pair(source, 1 - half).wait_recv()
        at = pl.ds(pl.multiple_of(source * M, M), M)

        def one(r, _):
            q_at = pl.ds(pl.multiple_of(r * BLOCK, BLOCK), BLOCK)
            scores = lax.dot_general(
                Q[q_at, :], KV[0, at, :], NT, preferred_element_type=jnp.float32
            )
            old = best[q_at, :]
            fresh = jnp.maximum(old, jnp.max(scores, axis=-1, keepdims=True))
            shrink = jnp.exp2(old - fresh)
            exponentials = jnp.exp2(scores - fresh)
            best[q_at, :] = fresh
            total[q_at, :] = total[q_at, :] * shrink + jnp.sum(exponentials, axis=-1, keepdims=True)
            summed[q_at, :] = summed[q_at, :] * shrink + jnp.dot(
                exponentials.astype(jnp.bfloat16), KV[1, at, :], preferred_element_type=jnp.float32
            )
            return 0

        lax.fori_loop(0, heads * M // BLOCK, one, 0, unroll=True)

    def both_ways(act, d):
        @pl.when(line >= d)
        def _():
            act(line - d)

        @pl.when(line + d < L)
        def _():
            act(line + d)

    kv_push(line, 0)
    kv_push(line, 1)
    kv_pair(line, half).start()

    def weight_step(d, _):
        kv_step(d - 1)
        weights.step(d)
        return 0

    lax.fori_loop(2, L - 1, weight_step, 0)
    kv_step(L - 2)
    outs.push_own()
    outs.push_pair()
    weights.step(L - 1)
    weights.local().wait()
    outs.local().wait()
    for rb in range(M // BLOCK):
        at = pl.ds(rb * BLOCK, BLOCK)
        raw = jnp.dot(X[at, :], W[...], preferred_element_type=jnp.float32).astype(jnp.bfloat16)
        for j in range(heads):
            part = raw[:, j * HEAD_DIM : (j + 1) * HEAD_DIM].astype(jnp.float32)
            Q[pl.ds(j * M + rb * BLOCK, BLOCK), :] = turned(part, qg_ref[...] * factor, at)

    attend(line)
    both_ways(attend, 1)
    outs.step(1)

    def attend_round(d, _):
        both_ways(attend, d)
        return 0

    lax.fori_loop(2, L - 1, attend_round, 0)
    kv_step(L - 1)
    both_ways(attend, L - 1)

    for ph in range(2):
        for pt in range(T):
            source = (ph * T + pt) * R
            target = (pt % 2) * T * R + (ph * H + pt // 2) * R
            for j in range(heads):
                at = pl.ds(j * M + source, R)
                A[pl.ds(target, R), j * HEAD_DIM : (j + 1) * HEAD_DIM] = (
                    summed[at, :] / total[at, :]
                ).astype(jnp.bfloat16)

    TR = T * R
    width = 2 * oc

    def product(parity, g):
        return lax.dot_general(
            A[pl.ds(pl.multiple_of(parity * TR, TR), TR), :],
            OW[pl.ds(pl.multiple_of(g * width, width), width), :],
            NT,
            preferred_element_type=jnp.float32,
        )

    def to_mate(g):
        return remote(SB.at[g], RC.at[g], cs_sem.at[g], cr_sem.at[g], (s, mate))

    def final_send(g, i):
        ph, pt = peer(lax.rem(h + i, T))
        return remote(
            SF.at[g, i - 1], RF.at[g, i - 1], fs_sem.at[g, i - 1], fr_sem.at[g, i - 1],
            (2 * line + ph, pt),
        )

    def reduced(g, hh):
        at = pl.ds(pl.multiple_of(hh * R, R), R)
        return PS[g, at, :] + RC[g, at, :].astype(jnp.float32)

    def multiply(g):
        SB[g] = product(1 - core, g).astype(jnp.bfloat16)
        to_mate(g).start()
        PS[g] = product(core, g)

    def spread(g):
        to_mate(g).wait_recv()
        for i in range(1, T):
            SF[g, i - 1] = reduced(g, lax.rem(h + i, T)).astype(jnp.bfloat16)
            final_send(g, i).start()

    multiply(line)
    both_ways(multiply, 1)
    spread(line)

    def out_round(d, _):
        both_ways(spread, d - 1)
        outs.step(d)
        both_ways(multiply, d)
        return 0

    lax.fori_loop(2, L, out_round, 0)
    both_ways(spread, L - 1)

    def gather_group(g, squares):
        result = reduced(g, h)
        for i in range(1, T):
            final_send(g, i).wait_recv()
            result = result + RF[g, i - 1].astype(jnp.float32)
        PS[g, pl.ds(pl.multiple_of(h * R, R), R), :] = result
        return squares + jnp.sum(result * result, axis=-1, keepdims=True)

    squares = lax.fori_loop(0, L, gather_group, jnp.zeros((R, 1), jnp.float32))
    norm = lax.rsqrt(squares / D + eps)
    for g in range(L):
        out_ref[:, g * width : (g + 1) * width] = (
            PS[g, pl.ds(pl.multiple_of(h * R, R), R), :] * norm
        ).astype(out_ref.dtype)

    kv_weights.finish()
    weights.finish()
    outs.finish()
    for i in range(1, T):
        token_send(i).wait_send()
    for i in range(T):
        token_mate(i).wait_send()

    def group_done(g, _):
        to_mate(g).wait_send()
        for i in range(1, T):
            final_send(g, i).wait_send()
        return 0

    lax.fori_loop(0, L, group_done, 0)

    def kv_done(source, _):
        kv_pair(source, half).wait_send()

        @pl.when((source <= line) & (line < L - 1))
        def _():
            kv_along(source, 1).wait_send()

        @pl.when((source >= line) & (line > 0))
        def _():
            kv_along(source, 0).wait_send()

        return 0

    lax.fori_loop(0, L, kv_done, 0)


def per_device(tokens, query_weight, key_weight, value_weight, out_weight, query_gain, key_gain):
    S, T = lax.axis_size("sp"), lax.axis_size("tp")
    L = S // 2
    R, D = tokens.shape
    M = 2 * T * R
    hw = query_weight.shape[1] // 2
    heads = hw // HEAD_DIM
    wr, oc = query_weight.shape[0], out_weight.shape[1]
    w = jnp.stack([query_weight[:, :hw], query_weight[:, hw:]])
    v = jnp.stack([key_weight, value_weight])
    o = jnp.swapaxes(out_weight.reshape(2, hw, oc), 1, 2)
    vmem = pl.BlockSpec(memory_space=pltpu.VMEM)
    bf, f32 = jnp.bfloat16, jnp.float32
    dma = pltpu.SemaphoreType.DMA
    return pl.pallas_call(
        functools.partial(kernel, S, T),
        out_shape=jax.ShapeDtypeStruct((R, D), bf),
        in_specs=[vmem] * 6,
        out_specs=vmem,
        scratch_shapes=[
            pltpu.VMEM((M, D), bf),
            pltpu.VMEM((S * wr, hw), bf),
            pltpu.VMEM((S * wr, HEAD_DIM), bf),
            pltpu.VMEM((S * oc, hw), bf),
            pltpu.VMEM((2, L * M, HEAD_DIM), bf),
            pltpu.VMEM((heads * M, HEAD_DIM), bf),
            pltpu.VMEM((M, hw), bf),
            pltpu.VMEM((M, HEAD_DIM), f32),
            pltpu.VMEM((M, HEAD_DIM), f32),
            pltpu.VMEM((heads * M, 1), f32),
            pltpu.VMEM((heads * M, 1), f32),
            pltpu.VMEM((heads * M, HEAD_DIM), f32),
            pltpu.VMEM((L, T * R, 2 * oc), f32),
            pltpu.VMEM((L, T * R, 2 * oc), bf),
            pltpu.VMEM((L, T * R, 2 * oc), bf),
            pltpu.VMEM((L, T - 1, R, 2 * oc), bf),
            pltpu.VMEM((L, T - 1, R, 2 * oc), bf),
            dma((2 * T,)),
            dma((2 * T,)),
            dma((3, S)),
            dma((S,)),
            dma((3, S)),
            dma((S,)),
            dma((3, S)),
            dma((S,)),
            dma((2, L)),
            dma((L,)),
            dma((L,)),
            dma((L,)),
            dma((L,)),
            dma((L,)),
            dma((L, T - 1)),
            dma((L, T - 1)),
        ],
        compiler_params=pltpu.CompilerParams(collective_id=0, has_side_effects=True),
    )(tokens, w, v, o, query_gain.reshape(1, HEAD_DIM), key_gain.reshape(1, HEAD_DIM))


def solution(mesh):
    placed = (
        P(("sp", "tp"), None),
        P("sp", "tp"),
        P("sp", "tp"),
        P("sp", "tp"),
        P("tp", "sp"),
        P(),
        P(),
    )
    return jax.shard_map(
        per_device, mesh=mesh, in_specs=placed, out_specs=P(("sp", "tp"), None), check_vma=False
    )
```

```python
import functools
import math

import jax
import jax.numpy as jnp
from jax import lax
from jax.experimental import pallas as pl
from jax.experimental.pallas import tpu as pltpu
from jax.sharding import PartitionSpec as P

HEAD_DIM = 128
GRID_W = 64
MESH = pl.DeviceIdType.MESH

eps = 1e-06
rope_base = 10000.0
BLOCK = 256
NT = (((1,), (1,)), ((), ()))


def remote(src, dst, send_sem, recv_sem, device):
    return pltpu.make_async_remote_copy(
        src_ref=src,
        dst_ref=dst,
        send_sem=send_sem,
        recv_sem=recv_sem,
        device_id=device,
        device_id_type=MESH,
    )


class Line:
    def __init__(self, own, buffer, size, send, recv, s, t, lines):
        self.own, self.buffer, self.size = own, buffer, size
        self.send, self.recv, self.s, self.t, self.lines = send, recv, s, t, lines
        self.line, self.half = s // 2, lax.rem(s, 2)

    def place(self, source):
        return self.buffer.at[pl.ds(pl.multiple_of(source * self.size, self.size), self.size)]

    def along(self, source, way, src=None):
        where = self.place(source)
        return remote(
            where if src is None else src,
            where,
            self.send.at[way, source],
            self.recv.at[source],
            (self.s + (2 if way else -2), self.t),
        )

    def push(self, source, way, src=None):
        @pl.when(self.line < self.lines - 1 if way else self.line > 0)
        def _():
            self.along(source, way, src).start()

    def each(self, which, act):
        if isinstance(self.own, tuple):
            for k, ref in enumerate(self.own):

                @pl.when(which == k)
                def _():
                    act(ref)

        else:
            act(self.own(which))

    def any_own(self):
        return self.own[0] if isinstance(self.own, tuple) else self.own(0)

    def pair(self, src=None):
        return remote(
            self.any_own() if src is None else src,
            self.place(self.s),
            self.send.at[2, self.s],
            self.recv.at[self.s],
            (self.s + 1 - 2 * self.half, self.t),
        )

    def local(self, src=None):
        return pltpu.make_async_copy(
            self.any_own() if src is None else src,
            self.place(self.s),
            self.send.at[2, self.s + 1 - 2 * self.half],
        )

    def push_pair_own(self):
        self.each(1 - self.half, lambda src: self.pair(src).start())

    def keep_own(self):
        self.each(self.half, lambda src: self.local(src).start())

    def push_own(self):
        self.each(self.half, lambda src: (self.push(self.s, 0, src), self.push(self.s, 1, src)))

    def arrived(self, source):
        self.along(source, 0).wait_recv()

    def push_pair(self):
        other = self.s + 1 - 2 * self.half
        self.arrived(other)
        self.push(other, 0)
        self.push(other, 1)

    def step(self, distance):
        for j in range(2):
            @pl.when(self.line >= distance)
            def _():
                source = 2 * (self.line - distance) + j
                self.arrived(source)
                self.push(source, 1)

            @pl.when(self.line + distance < self.lines)
            def _():
                source = 2 * (self.line + distance) + j
                self.arrived(source)
                self.push(source, 0)

    def finish(self):
        self.pair().wait_send()

        def one(source, _):
            @pl.when((source // 2 <= self.line) & (self.line < self.lines - 1))
            def _():
                self.along(source, 1).wait_send()

            @pl.when((source // 2 >= self.line) & (self.line > 0))
            def _():
                self.along(source, 0).wait_send()

            return 0

        lax.fori_loop(0, 2 * self.lines, one, 0)


def kernel(
    S, T,
    x_ref, w_ref, k_ref, v_ref, o_ref, qg_ref, kg_ref, out_ref,
    X, W, WV, OT, OW, KV, Q, A, C, SN, best, total, summed, PS, SB, RC, SF, RF,
    xs_sem, xr_sem, ws_sem, wr_sem, vs_sem, vr_sem, os_sem, or_sem, ks_sem, kr_sem, kp_sem, kq_sem,
    cs_sem, cr_sem, fs_sem, fr_sem,
):
    L, N = S // 2, 2 * T
    R, D = x_ref.shape
    M = N * R
    wr = w_ref.shape[0]
    hw, oc = o_ref.shape[0] // 2, o_ref.shape[1]
    heads = hw // HEAD_DIM
    s, t = lax.axis_index("sp"), lax.axis_index("tp")
    line, half = s // 2, lax.rem(s, 2)
    core, across = lax.rem(t, 2), t // 2
    mate = t + 1 - 2 * core
    other = s + 1 - 2 * half
    H = T // 2
    slot = half * T + t
    h = half * H + across

    def plane(b):
        return (2 * line + b // T, lax.rem(b, T))

    barrier = pltpu.get_barrier_semaphore()
    for i in range(1, N):
        pl.semaphore_signal(
            barrier, inc=1, device_id=plane(lax.rem(slot + i, N)), device_id_type=MESH
        )

    @pl.when(line > 0)
    def _():
        pl.semaphore_signal(barrier, inc=1, device_id=(s - 2, t), device_id_type=MESH)

    @pl.when(line < L - 1)
    def _():
        pl.semaphore_signal(barrier, inc=1, device_id=(s + 2, t), device_id_type=MESH)

    pl.semaphore_wait(
        barrier,
        N - 1 + jnp.where(line > 0, 1, 0) + jnp.where(line < L - 1, 1, 0),
    )

    weights = Line(lambda k: w_ref.at[:, pl.ds(pl.multiple_of(k * hw, hw), hw)], W, wr, ws_sem, wr_sem, s, t, L)
    kv_weights = Line((k_ref, v_ref), WV, wr, vs_sem, vr_sem, s, t, L)
    outs = Line(lambda k: OT.at[k], OW, oc, os_sem, or_sem, s, t, L)

    def rows(b):
        return X.at[pl.ds(pl.multiple_of(b * R, R), R)]

    def peer(hh):
        return hh // H, 2 * lax.rem(hh, H) + core

    def token_send(i):
        ph, pt = peer(lax.rem(h + i, T))
        return remote(x_ref, rows(slot), xs_sem.at[i], xr_sem.at[slot], (2 * line + ph, pt))

    def token_block(i):
        ph, pt = peer(lax.rem(h + T - i, T))
        return ph * T + pt

    def token_mate(i):
        b = token_block(i)
        return remote(
            x_ref if i == 0 else rows(b), rows(b), xs_sem.at[T + i], xr_sem.at[b], (s, mate)
        )

    kv_weights.push_pair_own()
    kv_weights.push_own()
    weights.push_pair_own()
    for i in range(1, T):
        token_send(i).start()
    token_mate(0).start()
    for k in range(2):
        OT[k] = o_ref[k * hw : (k + 1) * hw, :].T
    kv_weights.keep_own()
    weights.keep_own()
    own_tokens = pltpu.make_async_copy(x_ref, rows(slot), xs_sem.at[0])
    own_tokens.start()

    lane = lax.broadcasted_iota(jnp.int32, (BLOCK, HEAD_DIM), 1)
    pairs = HEAD_DIM // 4
    rate = jnp.exp(
        lax.rem(lane, pairs).astype(jnp.float32) * (-math.log(rope_base) / pairs)
    )
    by_row = lane < 2 * pairs
    leading = lax.rem(lane, 2 * pairs) < pairs
    for rb in range(M // BLOCK):
        position = (
            line * M + rb * BLOCK + lax.broadcasted_iota(jnp.int32, (BLOCK, HEAD_DIM), 0)
        )
        grid = jnp.where(by_row, position // GRID_W, lax.rem(position, GRID_W))
        angle = grid.astype(jnp.float32) * rate
        C[pl.ds(rb * BLOCK, BLOCK), :] = jnp.cos(angle)
        sine = jnp.sin(angle)
        SN[pl.ds(rb * BLOCK, BLOCK), :] = jnp.where(leading, -sine, sine)
    best[...] = jnp.full_like(best, -jnp.inf)
    total[...] = jnp.zeros_like(total)
    summed[...] = jnp.zeros_like(summed)

    outs.push_pair_own()
    outs.keep_own()
    kv_weights.push_pair()

    def kv_weight_step(d, _):
        kv_weights.step(d)
        return 0

    lax.fori_loop(1, L - 1, kv_weight_step, 0)
    weights.push_own()
    weights.push_pair()
    kv_weights.step(L - 1)
    for i in range(1, T):
        remote(x_ref, rows(token_block(i)), xs_sem.at[i], xr_sem.at[token_block(i)], (s, mate)).wait_recv()
        token_mate(i).start()

    weights.step(1)
    own_tokens.wait()
    kv_weights.local().wait()

    def mate_block(i):
        hh = lax.rem(h + T - i, T)
        return (hh // H) * T + 2 * lax.rem(hh, H) + 1 - core

    for i in range(T):
        b = mate_block(i)
        remote(x_ref, rows(b), xs_sem.at[i], xr_sem.at[b], (s, mate)).wait_recv()

    def turned(raw, gain, at):
        n = raw * lax.rsqrt(jnp.mean(raw * raw, axis=-1, keepdims=True) + eps) * gain
        partner = jnp.where(
            leading, pltpu.roll(n, HEAD_DIM - pairs, 1), pltpu.roll(n, pairs, 1)
        )
        return (n * C[at, :] + partner * SN[at, :]).astype(jnp.bfloat16)

    for rb in range(M // BLOCK):
        at = pl.ds(rb * BLOCK, BLOCK)
        kv = jnp.dot(X[at, :], WV[...], preferred_element_type=jnp.float32).astype(jnp.bfloat16)
        mine = pl.ds(pl.multiple_of(line * M + rb * BLOCK, BLOCK), BLOCK)

        @pl.when(half == 0)
        def _():
            KV[0, mine, :] = turned(kv.astype(jnp.float32), kg_ref[...], at)

        @pl.when(half == 1)
        def _():
            KV[1, mine, :] = kv

    def chunk(which, source):
        return KV.at[which, pl.ds(pl.multiple_of(source * M, M), M)]

    def kv_along(source, way):
        return remote(
            chunk(half, source), chunk(half, source), ks_sem.at[way, source], kr_sem.at[source],
            (s + (2 if way else -2), t),
        )

    def kv_pair(source, which):
        return remote(
            chunk(which, source), chunk(which, source), kp_sem.at[source], kq_sem.at[source],
            (other, t),
        )

    def kv_push(source, way):
        @pl.when(line < L - 1 if way else line > 0)
        def _():
            kv_along(source, way).start()

    def kv_step(d):
        for way in (1, 0):
            source = line - d if way else line + d

            @pl.when(line >= d if way else line + d < L)
            def _():
                kv_along(source, way).wait_recv()
                kv_push(source, way)
                kv_pair(source, half).start()

    factor = HEAD_DIM ** (-0.5) * math.log2(math.e)

    def attend(source):
        kv_pair(source, 1 - half).wait_recv()
        at = pl.ds(pl.multiple_of(source * M, M), M)

        def one(r, _):
            q_at = pl.ds(pl.multiple_of(r * BLOCK, BLOCK), BLOCK)
            scores = lax.dot_general(
                Q[q_at, :], KV[0, at, :], NT, preferred_element_type=jnp.float32
            )
            old = best[q_at, :]
            fresh = jnp.maximum(old, jnp.max(scores, axis=-1, keepdims=True))
            shrink = jnp.exp2(old - fresh)
            exponentials = jnp.exp2(scores - fresh)
            best[q_at, :] = fresh
            total[q_at, :] = total[q_at, :] * shrink + jnp.sum(exponentials, axis=-1, keepdims=True)
            summed[q_at, :] = summed[q_at, :] * shrink + jnp.dot(
                exponentials.astype(jnp.bfloat16), KV[1, at, :], preferred_element_type=jnp.float32
            )
            return 0

        lax.fori_loop(0, heads * M // BLOCK, one, 0, unroll=True)

    def both_ways(act, d):
        @pl.when(line >= d)
        def _():
            act(line - d)

        @pl.when(line + d < L)
        def _():
            act(line + d)

    kv_push(line, 0)
    kv_push(line, 1)
    kv_pair(line, half).start()

    def weight_step(d, _):
        kv_step(d - 1)
        weights.step(d)
        return 0

    lax.fori_loop(2, L - 1, weight_step, 0)
    kv_step(L - 2)
    outs.push_own()
    outs.push_pair()
    weights.step(L - 1)
    weights.local().wait()
    outs.local().wait()
    for rb in range(M // BLOCK):
        at = pl.ds(rb * BLOCK, BLOCK)
        raw = jnp.dot(X[at, :], W[...], preferred_element_type=jnp.float32).astype(jnp.bfloat16)
        for j in range(heads):
            part = raw[:, j * HEAD_DIM : (j + 1) * HEAD_DIM].astype(jnp.float32)
            Q[pl.ds(j * M + rb * BLOCK, BLOCK), :] = turned(part, qg_ref[...] * factor, at)

    attend(line)
    both_ways(attend, 1)
    outs.step(1)

    def attend_round(d, _):
        both_ways(attend, d)
        return 0

    lax.fori_loop(2, L - 1, attend_round, 0)
    kv_step(L - 1)
    both_ways(attend, L - 1)

    for ph in range(2):
        for pt in range(T):
            source = (ph * T + pt) * R
            target = (pt % 2) * T * R + (ph * H + pt // 2) * R
            for j in range(heads):
                at = pl.ds(j * M + source, R)
                A[pl.ds(target, R), j * HEAD_DIM : (j + 1) * HEAD_DIM] = (
                    summed[at, :] / total[at, :]
                ).astype(jnp.bfloat16)

    TR = T * R
    width = 2 * oc

    def product(parity, g):
        return lax.dot_general(
            A[pl.ds(pl.multiple_of(parity * TR, TR), TR), :],
            OW[pl.ds(pl.multiple_of(g * width, width), width), :],
            NT,
            preferred_element_type=jnp.float32,
        )

    def to_mate(g):
        return remote(SB.at[g], RC.at[g], cs_sem.at[g], cr_sem.at[g], (s, mate))

    def final_send(g, i):
        ph, pt = peer(lax.rem(h + i, T))
        return remote(
            SF.at[g, i - 1], RF.at[g, i - 1], fs_sem.at[g, i - 1], fr_sem.at[g, i - 1],
            (2 * line + ph, pt),
        )

    def reduced(g, hh):
        at = pl.ds(pl.multiple_of(hh * R, R), R)
        return PS[g, at, :] + RC[g, at, :].astype(jnp.float32)

    def multiply(g):
        SB[g] = product(1 - core, g).astype(jnp.bfloat16)
        to_mate(g).start()
        PS[g] = product(core, g)

    def spread(g):
        to_mate(g).wait_recv()
        for i in range(1, T):
            SF[g, i - 1] = reduced(g, lax.rem(h + i, T)).astype(jnp.bfloat16)
            final_send(g, i).start()

    multiply(line)
    both_ways(multiply, 1)
    spread(line)

    def out_round(d, _):
        both_ways(spread, d - 1)
        outs.step(d)
        both_ways(multiply, d)
        return 0

    lax.fori_loop(2, L, out_round, 0)
    both_ways(spread, L - 1)

    def gather_group(g, squares):
        result = reduced(g, h)
        for i in range(1, T):
            final_send(g, i).wait_recv()
            result = result + RF[g, i - 1].astype(jnp.float32)
        PS[g, pl.ds(pl.multiple_of(h * R, R), R), :] = result
        return squares + jnp.sum(result * result, axis=-1, keepdims=True)

    squares = lax.fori_loop(0, L, gather_group, jnp.zeros((R, 1), jnp.float32))
    norm = lax.rsqrt(squares / D + eps)
    for g in range(L):
        out_ref[:, g * width : (g + 1) * width] = (
            PS[g, pl.ds(pl.multiple_of(h * R, R), R), :] * norm
        ).astype(out_ref.dtype)

    kv_weights.finish()
    weights.finish()
    outs.finish()
    for i in range(1, T):
        token_send(i).wait_send()
    for i in range(T):
        token_mate(i).wait_send()

    def group_done(g, _):
        to_mate(g).wait_send()
        for i in range(1, T):
            final_send(g, i).wait_send()
        return 0

    lax.fori_loop(0, L, group_done, 0)

    def kv_done(source, _):
        kv_pair(source, half).wait_send()

        @pl.when((source <= line) & (line < L - 1))
        def _():
            kv_along(source, 1).wait_send()

        @pl.when((source >= line) & (line > 0))
        def _():
            kv_along(source, 0).wait_send()

        return 0

    lax.fori_loop(0, L, kv_done, 0)


def per_device(tokens, query_weight, key_weight, value_weight, out_weight, query_gain, key_gain):
    S, T = lax.axis_size("sp"), lax.axis_size("tp")
    L = S // 2
    R, D = tokens.shape
    M = 2 * T * R
    hw = query_weight.shape[1] // 2
    heads = hw // HEAD_DIM
    wr, oc = query_weight.shape[0], out_weight.shape[1]
    vmem = pl.BlockSpec(memory_space=pltpu.VMEM)
    bf, f32 = jnp.bfloat16, jnp.float32
    dma = pltpu.SemaphoreType.DMA
    return pl.pallas_call(
        functools.partial(kernel, S, T),
        out_shape=jax.ShapeDtypeStruct((R, D), bf),
        in_specs=[vmem] * 7,
        out_specs=vmem,
        scratch_shapes=[
            pltpu.VMEM((M, D), bf),
            pltpu.VMEM((S * wr, hw), bf),
            pltpu.VMEM((S * wr, HEAD_DIM), bf),
            pltpu.VMEM((2, oc, hw), bf),
            pltpu.VMEM((S * oc, hw), bf),
            pltpu.VMEM((2, L * M, HEAD_DIM), bf),
            pltpu.VMEM((heads * M, HEAD_DIM), bf),
            pltpu.VMEM((M, hw), bf),
            pltpu.VMEM((M, HEAD_DIM), f32),
            pltpu.VMEM((M, HEAD_DIM), f32),
            pltpu.VMEM((heads * M, 1), f32),
            pltpu.VMEM((heads * M, 1), f32),
            pltpu.VMEM((heads * M, HEAD_DIM), f32),
            pltpu.VMEM((L, T * R, 2 * oc), f32),
            pltpu.VMEM((L, T * R, 2 * oc), bf),
            pltpu.VMEM((L, T * R, 2 * oc), bf),
            pltpu.VMEM((L, T - 1, R, 2 * oc), bf),
            pltpu.VMEM((L, T - 1, R, 2 * oc), bf),
            dma((2 * T,)),
            dma((2 * T,)),
            dma((3, S)),
            dma((S,)),
            dma((3, S)),
            dma((S,)),
            dma((3, S)),
            dma((S,)),
            dma((2, L)),
            dma((L,)),
            dma((L,)),
            dma((L,)),
            dma((L,)),
            dma((L,)),
            dma((L, T - 1)),
            dma((L, T - 1)),
        ],
        compiler_params=pltpu.CompilerParams(collective_id=0, has_side_effects=True),
    )(
        tokens, query_weight, key_weight, value_weight, out_weight,
        query_gain.reshape(1, HEAD_DIM), key_gain.reshape(1, HEAD_DIM),
    )


def solution(mesh):
    placed = (
        P(("sp", "tp"), None),
        P("sp", "tp"),
        P("sp", "tp"),
        P("sp", "tp"),
        P("tp", "sp"),
        P(),
        P(),
    )
    return jax.shard_map(
        per_device, mesh=mesh, in_specs=placed, out_specs=P(("sp", "tp"), None), check_vma=False
    )
```

```python
import functools
import math

import jax
import jax.numpy as jnp
from jax import lax
from jax.experimental import pallas as pl
from jax.experimental.pallas import tpu as pltpu
from jax.sharding import PartitionSpec as P

HEAD_DIM = 128
GRID_W = 64
MESH = pl.DeviceIdType.MESH

eps = 1e-06
rope_base = 10000.0
BLOCK = 256
NT = (((1,), (1,)), ((), ()))


def remote(src, dst, send_sem, recv_sem, device):
    return pltpu.make_async_remote_copy(
        src_ref=src,
        dst_ref=dst,
        send_sem=send_sem,
        recv_sem=recv_sem,
        device_id=device,
        device_id_type=MESH,
    )


class Line:
    def __init__(self, own, buffer, size, send, recv, s, t, lines):
        self.own, self.buffer, self.size = own, buffer, size
        self.send, self.recv, self.s, self.t, self.lines = send, recv, s, t, lines
        self.line, self.half = s // 2, lax.rem(s, 2)

    def place(self, source):
        return self.buffer.at[pl.ds(pl.multiple_of(source * self.size, self.size), self.size)]

    def along(self, source, way, src=None):
        where = self.place(source)
        return remote(
            where if src is None else src,
            where,
            self.send.at[way, source],
            self.recv.at[source],
            (self.s + (2 if way else -2), self.t),
        )

    def push(self, source, way, src=None):
        @pl.when(self.line < self.lines - 1 if way else self.line > 0)
        def _():
            self.along(source, way, src).start()

    def each(self, which, act):
        if isinstance(self.own, tuple):
            for k, ref in enumerate(self.own):

                @pl.when(which == k)
                def _():
                    act(ref)

        else:
            act(self.own(which))

    def any_own(self):
        return self.own[0] if isinstance(self.own, tuple) else self.own(0)

    def pair(self, src=None):
        return remote(
            self.any_own() if src is None else src,
            self.place(self.s),
            self.send.at[2, self.s],
            self.recv.at[self.s],
            (self.s + 1 - 2 * self.half, self.t),
        )

    def local(self, src=None):
        return pltpu.make_async_copy(
            self.any_own() if src is None else src,
            self.place(self.s),
            self.send.at[2, self.s + 1 - 2 * self.half],
        )

    def push_pair_own(self):
        self.each(1 - self.half, lambda src: self.pair(src).start())

    def keep_own(self):
        self.each(self.half, lambda src: self.local(src).start())

    def push_own(self):
        self.each(self.half, lambda src: (self.push(self.s, 0, src), self.push(self.s, 1, src)))

    def arrived(self, source):
        self.along(source, 0).wait_recv()

    def push_pair(self):
        other = self.s + 1 - 2 * self.half
        self.arrived(other)
        self.push(other, 0)
        self.push(other, 1)

    def step(self, distance):
        for j in range(2):
            @pl.when(self.line >= distance)
            def _():
                source = 2 * (self.line - distance) + j
                self.arrived(source)
                self.push(source, 1)

            @pl.when(self.line + distance < self.lines)
            def _():
                source = 2 * (self.line + distance) + j
                self.arrived(source)
                self.push(source, 0)

    def finish(self):
        self.pair().wait_send()

        def one(source, _):
            @pl.when((source // 2 <= self.line) & (self.line < self.lines - 1))
            def _():
                self.along(source, 1).wait_send()

            @pl.when((source // 2 >= self.line) & (self.line > 0))
            def _():
                self.along(source, 0).wait_send()

            return 0

        lax.fori_loop(0, 2 * self.lines, one, 0)


def kernel(
    S, T,
    x_ref, w_ref, k_ref, v_ref, o_ref, qg_ref, kg_ref, out_ref,
    X, W, WV, OT, OW, KV, Q, A, C, SN, best, total, summed, PS, SB, RC, SF, RF,
    xs_sem, xr_sem, ws_sem, wr_sem, vs_sem, vr_sem, os_sem, or_sem, ks_sem, kr_sem, kp_sem, kq_sem,
    cs_sem, cr_sem, fs_sem, fr_sem,
):
    L, N = S // 2, 2 * T
    R, D = x_ref.shape
    M = N * R
    wr = w_ref.shape[0]
    hw, oc = o_ref.shape[0] // 2, o_ref.shape[1]
    heads = hw // HEAD_DIM
    s, t = lax.axis_index("sp"), lax.axis_index("tp")
    line, half = s // 2, lax.rem(s, 2)
    core, across = lax.rem(t, 2), t // 2
    mate = t + 1 - 2 * core
    other = s + 1 - 2 * half
    H = T // 2
    slot = half * T + t
    h = half * H + across

    def plane(b):
        return (2 * line + b // T, lax.rem(b, T))

    barrier = pltpu.get_barrier_semaphore()
    for i in range(1, N):
        pl.semaphore_signal(
            barrier, inc=1, device_id=plane(lax.rem(slot + i, N)), device_id_type=MESH
        )

    @pl.when(line > 0)
    def _():
        pl.semaphore_signal(barrier, inc=1, device_id=(s - 2, t), device_id_type=MESH)

    @pl.when(line < L - 1)
    def _():
        pl.semaphore_signal(barrier, inc=1, device_id=(s + 2, t), device_id_type=MESH)

    pl.semaphore_wait(
        barrier,
        N - 1 + jnp.where(line > 0, 1, 0) + jnp.where(line < L - 1, 1, 0),
    )

    weights = Line(lambda k: w_ref.at[:, pl.ds(pl.multiple_of(k * hw, hw), hw)], W, wr, ws_sem, wr_sem, s, t, L)
    kv_weights = Line((k_ref, v_ref), WV, wr, vs_sem, vr_sem, s, t, L)
    outs = Line(lambda k: OT.at[k], OW, oc, os_sem, or_sem, s, t, L)

    def rows(b):
        return X.at[pl.ds(pl.multiple_of(b * R, R), R)]

    def peer(hh):
        return hh // H, 2 * lax.rem(hh, H) + core

    def token_send(i):
        ph, pt = peer(lax.rem(h + i, T))
        return remote(x_ref, rows(slot), xs_sem.at[i], xr_sem.at[slot], (2 * line + ph, pt))

    def token_block(i):
        ph, pt = peer(lax.rem(h + T - i, T))
        return ph * T + pt

    def token_mate(i):
        b = token_block(i)
        return remote(
            x_ref if i == 0 else rows(b), rows(b), xs_sem.at[T + i], xr_sem.at[b], (s, mate)
        )

    kv_weights.push_pair_own()
    kv_weights.push_own()
    weights.push_pair_own()
    for i in range(1, T):
        token_send(i).start()
    token_mate(0).start()
    for k in range(2):
        OT[k] = o_ref[k * hw : (k + 1) * hw, :].T
    kv_weights.keep_own()
    weights.keep_own()
    own_tokens = pltpu.make_async_copy(x_ref, rows(slot), xs_sem.at[0])
    own_tokens.start()

    lane = lax.broadcasted_iota(jnp.int32, (BLOCK, HEAD_DIM), 1)
    pairs = HEAD_DIM // 4
    rate = jnp.exp(
        lax.rem(lane, pairs).astype(jnp.float32) * (-math.log(rope_base) / pairs)
    )
    by_row = lane < 2 * pairs
    leading = lax.rem(lane, 2 * pairs) < pairs
    for rb in range(M // BLOCK):
        position = (
            line * M + rb * BLOCK + lax.broadcasted_iota(jnp.int32, (BLOCK, HEAD_DIM), 0)
        )
        grid = jnp.where(by_row, position // GRID_W, lax.rem(position, GRID_W))
        angle = grid.astype(jnp.float32) * rate
        C[pl.ds(rb * BLOCK, BLOCK), :] = jnp.cos(angle)
        sine = jnp.sin(angle)
        SN[pl.ds(rb * BLOCK, BLOCK), :] = jnp.where(leading, -sine, sine)
    best[...] = jnp.full_like(best, -jnp.inf)
    total[...] = jnp.zeros_like(total)
    summed[...] = jnp.zeros_like(summed)

    outs.push_pair_own()
    outs.keep_own()
    kv_weights.push_pair()

    def kv_weight_step(d, _):
        kv_weights.step(d)
        return 0

    lax.fori_loop(1, L - 1, kv_weight_step, 0)
    weights.push_own()
    weights.push_pair()
    kv_weights.step(L - 1)
    for i in range(1, T):
        remote(x_ref, rows(token_block(i)), xs_sem.at[i], xr_sem.at[token_block(i)], (s, mate)).wait_recv()
        token_mate(i).start()

    weights.step(1)
    own_tokens.wait()
    kv_weights.local().wait()

    def mate_block(i):
        hh = lax.rem(h + T - i, T)
        return (hh // H) * T + 2 * lax.rem(hh, H) + 1 - core

    for i in range(T):
        b = mate_block(i)
        remote(x_ref, rows(b), xs_sem.at[i], xr_sem.at[b], (s, mate)).wait_recv()

    def turned(raw, gain, at):
        n = raw * lax.rsqrt(jnp.mean(raw * raw, axis=-1, keepdims=True) + eps) * gain
        partner = jnp.where(
            leading, pltpu.roll(n, HEAD_DIM - pairs, 1), pltpu.roll(n, pairs, 1)
        )
        return (n * C[at, :] + partner * SN[at, :]).astype(jnp.bfloat16)

    for rb in range(M // BLOCK):
        at = pl.ds(rb * BLOCK, BLOCK)
        kv = jnp.dot(X[at, :], WV[...], preferred_element_type=jnp.float32).astype(jnp.bfloat16)
        mine = pl.ds(pl.multiple_of(line * M + rb * BLOCK, BLOCK), BLOCK)

        @pl.when(half == 0)
        def _():
            KV[0, mine, :] = turned(kv.astype(jnp.float32), kg_ref[...], at)

        @pl.when(half == 1)
        def _():
            KV[1, mine, :] = kv

    def chunk(which, source):
        return KV.at[which, pl.ds(pl.multiple_of(source * M, M), M)]

    def kv_along(source, way):
        return remote(
            chunk(half, source), chunk(half, source), ks_sem.at[way, source], kr_sem.at[source],
            (s + (2 if way else -2), t),
        )

    def kv_pair(source, which):
        return remote(
            chunk(which, source), chunk(which, source), kp_sem.at[source], kq_sem.at[source],
            (other, t),
        )

    def kv_push(source, way):
        @pl.when(line < L - 1 if way else line > 0)
        def _():
            kv_along(source, way).start()

    def kv_step(d):
        for way in (1, 0):
            source = line - d if way else line + d

            @pl.when(line >= d if way else line + d < L)
            def _():
                kv_along(source, way).wait_recv()
                kv_push(source, way)
                kv_pair(source, half).start()

    factor = HEAD_DIM ** (-0.5) * math.log2(math.e)

    def attend(source):
        kv_pair(source, 1 - half).wait_recv()
        at = pl.ds(pl.multiple_of(source * M, M), M)

        def one(r, _):
            q_at = pl.ds(pl.multiple_of(r * BLOCK, BLOCK), BLOCK)
            scores = lax.dot_general(
                Q[q_at, :], KV[0, at, :], NT, preferred_element_type=jnp.float32
            )
            old = best[q_at, :]
            fresh = jnp.maximum(old, jnp.max(scores, axis=-1, keepdims=True))
            shrink = jnp.exp2(old - fresh)
            exponentials = jnp.exp2(scores - fresh)
            best[q_at, :] = fresh
            total[q_at, :] = total[q_at, :] * shrink + jnp.sum(exponentials, axis=-1, keepdims=True)
            summed[q_at, :] = summed[q_at, :] * shrink + jnp.dot(
                exponentials.astype(jnp.bfloat16), KV[1, at, :], preferred_element_type=jnp.float32
            )
            return 0

        lax.fori_loop(0, heads * M // BLOCK, one, 0, unroll=True)

    def both_ways(act, d):
        @pl.when(line >= d)
        def _():
            act(line - d)

        @pl.when(line + d < L)
        def _():
            act(line + d)

    kv_push(line, 0)
    kv_push(line, 1)
    kv_pair(line, half).start()

    def weight_step(d, _):
        kv_step(d - 1)
        weights.step(d)
        return 0

    lax.fori_loop(2, L - 1, weight_step, 0)
    kv_step(L - 2)
    outs.push_own()
    outs.push_pair()
    weights.step(L - 1)
    weights.local().wait()
    outs.local().wait()
    for rb in range(M // BLOCK):
        at = pl.ds(rb * BLOCK, BLOCK)
        raw = jnp.dot(X[at, :], W[...], preferred_element_type=jnp.float32).astype(jnp.bfloat16)
        for j in range(heads):
            part = raw[:, j * HEAD_DIM : (j + 1) * HEAD_DIM].astype(jnp.float32)
            Q[pl.ds(j * M + rb * BLOCK, BLOCK), :] = turned(part, qg_ref[...] * factor, at)

    inner = (line > 0) & (line < L - 1)
    attend(line)
    outs.step(1)
    both_ways(attend, 1)

    @pl.when(inner)
    def _():
        def relay(d, _):
            outs.step(d)
            return 0

        lax.fori_loop(2, L, relay, 0)

    def attend_round(d, _):
        both_ways(attend, d)
        return 0

    lax.fori_loop(2, L - 1, attend_round, 0)
    kv_step(L - 1)
    both_ways(attend, L - 1)

    for ph in range(2):
        for pt in range(T):
            source = (ph * T + pt) * R
            target = (pt % 2) * T * R + (ph * H + pt // 2) * R
            for j in range(heads):
                at = pl.ds(j * M + source, R)
                A[pl.ds(target, R), j * HEAD_DIM : (j + 1) * HEAD_DIM] = (
                    summed[at, :] / total[at, :]
                ).astype(jnp.bfloat16)

    TR = T * R
    width = 2 * oc

    def product(parity, g):
        return lax.dot_general(
            A[pl.ds(pl.multiple_of(parity * TR, TR), TR), :],
            OW[pl.ds(pl.multiple_of(g * width, width), width), :],
            NT,
            preferred_element_type=jnp.float32,
        )

    def to_mate(g):
        return remote(SB.at[g], RC.at[g], cs_sem.at[g], cr_sem.at[g], (s, mate))

    def final_send(g, i):
        ph, pt = peer(lax.rem(h + i, T))
        return remote(
            SF.at[g, i - 1], RF.at[g, i - 1], fs_sem.at[g, i - 1], fr_sem.at[g, i - 1],
            (2 * line + ph, pt),
        )

    def reduced(g, hh):
        at = pl.ds(pl.multiple_of(hh * R, R), R)
        return PS[g, at, :] + RC[g, at, :].astype(jnp.float32)

    def multiply(g):
        SB[g] = product(1 - core, g).astype(jnp.bfloat16)
        to_mate(g).start()
        PS[g] = product(core, g)

    def spread(g):
        to_mate(g).wait_recv()
        for i in range(1, T):
            SF[g, i - 1] = reduced(g, lax.rem(h + i, T)).astype(jnp.bfloat16)
            final_send(g, i).start()

    multiply(line)
    both_ways(multiply, 1)
    spread(line)

    def out_round(d, _):
        both_ways(spread, d - 1)

        @pl.when(jnp.logical_not(inner))
        def _():
            outs.step(d)

        both_ways(multiply, d)
        return 0

    lax.fori_loop(2, L, out_round, 0)
    both_ways(spread, L - 1)

    def gather_group(g, squares):
        result = reduced(g, h)
        for i in range(1, T):
            final_send(g, i).wait_recv()
            result = result + RF[g, i - 1].astype(jnp.float32)
        PS[g, pl.ds(pl.multiple_of(h * R, R), R), :] = result
        return squares + jnp.sum(result * result, axis=-1, keepdims=True)

    squares = lax.fori_loop(0, L, gather_group, jnp.zeros((R, 1), jnp.float32))
    norm = lax.rsqrt(squares / D + eps)
    for g in range(L):
        out_ref[:, g * width : (g + 1) * width] = (
            PS[g, pl.ds(pl.multiple_of(h * R, R), R), :] * norm
        ).astype(out_ref.dtype)

    kv_weights.finish()
    weights.finish()
    outs.finish()
    for i in range(1, T):
        token_send(i).wait_send()
    for i in range(T):
        token_mate(i).wait_send()

    def group_done(g, _):
        to_mate(g).wait_send()
        for i in range(1, T):
            final_send(g, i).wait_send()
        return 0

    lax.fori_loop(0, L, group_done, 0)

    def kv_done(source, _):
        kv_pair(source, half).wait_send()

        @pl.when((source <= line) & (line < L - 1))
        def _():
            kv_along(source, 1).wait_send()

        @pl.when((source >= line) & (line > 0))
        def _():
            kv_along(source, 0).wait_send()

        return 0

    lax.fori_loop(0, L, kv_done, 0)


def per_device(tokens, query_weight, key_weight, value_weight, out_weight, query_gain, key_gain):
    S, T = lax.axis_size("sp"), lax.axis_size("tp")
    L = S // 2
    R, D = tokens.shape
    M = 2 * T * R
    hw = query_weight.shape[1] // 2
    heads = hw // HEAD_DIM
    wr, oc = query_weight.shape[0], out_weight.shape[1]
    vmem = pl.BlockSpec(memory_space=pltpu.VMEM)
    bf, f32 = jnp.bfloat16, jnp.float32
    dma = pltpu.SemaphoreType.DMA
    return pl.pallas_call(
        functools.partial(kernel, S, T),
        out_shape=jax.ShapeDtypeStruct((R, D), bf),
        in_specs=[vmem] * 7,
        out_specs=vmem,
        scratch_shapes=[
            pltpu.VMEM((M, D), bf),
            pltpu.VMEM((S * wr, hw), bf),
            pltpu.VMEM((S * wr, HEAD_DIM), bf),
            pltpu.VMEM((2, oc, hw), bf),
            pltpu.VMEM((S * oc, hw), bf),
            pltpu.VMEM((2, L * M, HEAD_DIM), bf),
            pltpu.VMEM((heads * M, HEAD_DIM), bf),
            pltpu.VMEM((M, hw), bf),
            pltpu.VMEM((M, HEAD_DIM), f32),
            pltpu.VMEM((M, HEAD_DIM), f32),
            pltpu.VMEM((heads * M, 1), f32),
            pltpu.VMEM((heads * M, 1), f32),
            pltpu.VMEM((heads * M, HEAD_DIM), f32),
            pltpu.VMEM((L, T * R, 2 * oc), f32),
            pltpu.VMEM((L, T * R, 2 * oc), bf),
            pltpu.VMEM((L, T * R, 2 * oc), bf),
            pltpu.VMEM((L, T - 1, R, 2 * oc), bf),
            pltpu.VMEM((L, T - 1, R, 2 * oc), bf),
            dma((2 * T,)),
            dma((2 * T,)),
            dma((3, S)),
            dma((S,)),
            dma((3, S)),
            dma((S,)),
            dma((3, S)),
            dma((S,)),
            dma((2, L)),
            dma((L,)),
            dma((L,)),
            dma((L,)),
            dma((L,)),
            dma((L,)),
            dma((L, T - 1)),
            dma((L, T - 1)),
        ],
        compiler_params=pltpu.CompilerParams(collective_id=0, has_side_effects=True),
    )(
        tokens, query_weight, key_weight, value_weight, out_weight,
        query_gain.reshape(1, HEAD_DIM), key_gain.reshape(1, HEAD_DIM),
    )


def solution(mesh):
    placed = (
        P(("sp", "tp"), None),
        P("sp", "tp"),
        P("sp", "tp"),
        P("sp", "tp"),
        P("tp", "sp"),
        P(),
        P(),
    )
    return jax.shard_map(
        per_device, mesh=mesh, in_specs=placed, out_specs=P(("sp", "tp"), None), check_vma=False
    )
```
